32 devices in a mesh: sp: 8 (over z, x), tp: 4 (over y, core).
Axes of the slice: x: 2, y: 2, z: 4, core: 2. Of those that a mesh axis runs over, the one named last changes fastest.
Arguments:
- x_in: bfloat16 [4096, 1024], P('sp', 'tp'), may hold values from -6 to 6
- gate_b: bfloat16 [4096, 1024], P('sp', 'tp'), may hold values from -6 to 6
- gate_c: bfloat16 [4096, 1024], P('sp', 'tp'), may hold values from -6 to 6
- conv_taps: bfloat16 [3, 1024], P(None, 'tp'), may hold values from -3.5 to 3.5
- out_proj: bfloat16 [1024, 2048], P('tp'), may hold values from -0.1875 to 0.1875
- mix_gain: bfloat16 [2048], replicated, may hold values from 0.099609375 to 1.8984375
- resid: bfloat16 [4096, 2048], P(('sp', 'tp')), may hold values from -6 to 6
- pre_gain: bfloat16 [2048], replicated, may hold values from 0.099609375 to 1.8984375
- expert_gate: bfloat16 [8, 2048, 512], P('sp'), may hold values from -0.125 to 0.125
- expert_up: bfloat16 [8, 2048, 512], P('sp'), may hold values from -0.125 to 0.125
- expert_down: bfloat16 [8, 512, 2048], P('sp'), may hold values from -7.1594562 to 7.1594562
- shared_gate: bfloat16 [2048, 256], replicated, may hold values from -0.125 to 0.125
- shared_up: bfloat16 [2048, 256], replicated, may hold values from -0.125 to 0.125
- shared_down: bfloat16 [256, 2048], replicated, may hold values from -10.125 to 10.125
- post_gain: bfloat16 [2048], replicated, may hold values from 0.099609375 to 1.8984375
- routes: int32 [4096, 4], P(('sp', 'tp')), may hold values from 0 to 7, all different within a row; in each aligned block of 128 rows (0 to 127, 128 to 255, ...) at most 96 rows name the same one
- route_weights: float32 [4096, 4], P(('sp', 'tp')), may hold values from 0.1 to 1
Outputs:
- layer_out: bfloat16 [4096, 2048], P(('sp', 'tp'))
The draws below stay inside these ranges and needn't reach their ends.
Inputs may be any that keep to these rules, and one draw needn't show every extreme that they name: `routes`: each row names 4 different experts. Within the rows of one device (aligned blocks), no expert is named by more than 96 rows, and in some block one expert is named by exactly 96 rows.
All inputs are finite; a program needn't handle non-finite values.
Results may differ from the reference program's by a relative error of at most 0.007.
Values may be sent and summed in bfloat16 or wider, within the bound.
A program may use at most 128 MiB of HBM per device.

```python
import math
import jax
import jax.numpy as jnp
import numpy as np
from jax import lax

D = 2048
CONV_CH = 1024
EXPERT_HIDDEN = 512
SHARED_HIDDEN = 256
CONV_WIDTH = 3
TOPK = 4
TOK_DEV = 512
EXPERTS = 8
CAP = 96
TOKENS = 4096
N_SP = 8
N_TP = 4


def column_scale(key, count):
    ramp = 3.0 ** (jnp.arange(count, dtype=jnp.float32) / count)
    rough = 10.0 ** jax.random.uniform(key, (count,), jnp.float32)
    return ramp * rough / 10.0


def draw_expert_down(key, part):
    first, second = jax.random.split(key)
    base = jnp.clip(jax.random.normal(first, (EXPERTS, EXPERT_HIDDEN, D), jnp.float32), -6.0, 6.0)
    return (base * EXPERT_HIDDEN ** (-0.5) * column_scale(second, D)[None, None, :]).astype(jnp.bfloat16)


def draw_shared_down(key, part):
    first, second = jax.random.split(key)
    base = jnp.clip(jax.random.normal(first, (SHARED_HIDDEN, D), jnp.float32), -6.0, 6.0)
    return (base * SHARED_HIDDEN ** (-0.5) * column_scale(second, D)[None, :]).astype(jnp.bfloat16)


def levels(rng, dims, shards, low, top_value):
    gain, own = 1.0, jax.random.fold_in(rng, 6)
    for dim, blocks in shards:
        steps = jnp.exp(jax.random.uniform(jax.random.fold_in(own, dim), (blocks,), jnp.float32, low / len(shards), top_value / len(shards)))
        gain = gain * jnp.repeat(steps, dims[dim] // blocks).reshape([-1 if axis == dim else 1 for axis in range(len(dims))])
    return gain


def assign_block(stream_key, own, number, rows, number_of, top, most, skew):
    order = jax.random.permutation(stream_key, number_of)
    packed, common = load_shares(number_of, rows * top, most, skew, True), load_shares(number_of, rows * top, most, skew, False)
    places = jnp.arange(number_of)

    def named(tallies, rotation):
        used = int((tallies > 0).sum())
        fixed = max(1, used // 4)
        moved = fixed + (places - fixed + rotation * (used - fixed)) % max(1, number_of - fixed)
        return jnp.zeros((number_of,), jnp.int32).at[order[jnp.where(places < fixed, places, moved)]].set(jnp.asarray(tallies, jnp.int32))

    tallies = jnp.where(number % 4 == 0, named(packed, number // 4), named(common, number - number // 4 - 1))
    mixed = jax.random.permutation(jax.random.fold_in(own, 3), number_of)
    giver, sink = mixed[0:number_of // 2 * 2:2], mixed[1:number_of // 2 * 2:2]
    margin = jnp.minimum(tallies[giver] - 1, most - tallies[sink]) // 2
    margin = jnp.where((giver == order[0]) | (sink == order[0]) | (tallies[sink] == 0), 0, jnp.maximum(margin, 0))
    moved = jax.random.randint(jax.random.fold_in(own, 4), (number_of // 2,), 0, 1 << 20) % (margin + 1)
    tallies = tallies.at[giver].add(-moved).at[sink].add(moved)
    members = jnp.searchsorted(jnp.cumsum(tallies), jnp.arange(rows * top), side="right").astype(jnp.int32)
    table = members.reshape(top, rows).T
    table = table[jax.random.permutation(jax.random.fold_in(own, 1), rows)]
    rotation = jax.random.randint(jax.random.fold_in(own, 2), (rows, 1), 0, top)
    return jnp.take_along_axis(table, (jnp.arange(top)[None, :] + rotation) % top, axis=1)


def load_shares(count, total, bound, lean, full):
    loads = [(1 << 20) // math.isqrt(grade ** lean) + 1 for grade in range(1, count + 1)]
    largest = bound if full else min(bound, max(-(-total // count), total * loads[0] // sum(loads)))
    least = 1 if total - largest >= count - 1 else 0
    holding, rest = [largest] + [least] * (count - 1), total - largest - least * (count - 1)
    while rest > 0:
        free = [i for i in range(1, count) if holding[i] < largest] or [i for i in range(1, count) if holding[i] < bound]
        whole, budget = sum([loads[i] for i in free]), rest
        for i in free:
            addition = min(bound - holding[i], max(1, budget * loads[i] // whole), rest)
            holding[i] = holding[i] + addition
            rest = rest - addition
    return np.array(holding)


def centred(own_key, extent, spread, most, pieces=(), kind=jnp.bfloat16):
    level = levels(own_key, extent, pieces, -0.22, 0.18) if pieces else 1.0
    array = jax.random.normal(own_key, extent, jnp.float32) * spread * level
    return jnp.minimum(jnp.maximum(array, -most), most).astype(kind)


def setup_inputs(seed: int = 0) -> dict:
    arg_keys = jax.random.split(jax.random.key(seed), 18)
    x_in = centred(arg_keys[0], (TOKENS, CONV_CH), 1.0, 6.0, ((0, 8), (1, 4)))
    gate_b = centred(arg_keys[1], (TOKENS, CONV_CH), 1.0, 6.0, ((0, 8), (1, 4)))
    gate_c = centred(arg_keys[2], (TOKENS, CONV_CH), 1.0, 6.0, ((0, 8), (1, 4)))
    conv_taps = centred(arg_keys[3], (CONV_WIDTH, CONV_CH), CONV_WIDTH ** -0.5, 3.5, ((1, 4),))
    out_proj = centred(arg_keys[4], (CONV_CH, D), CONV_CH ** -0.5, 0.1875, ((0, 4),))
    mix_gain = jnp.clip(1.0 + 0.18 * jax.random.normal(arg_keys[5], (D,), jnp.float32), 0.099609375, 1.8984375).astype(jnp.bfloat16)
    resid = centred(arg_keys[6], (TOKENS, D), 1.0, 6.0, ((0, 32),))
    pre_gain = jnp.clip(1.0 + 0.18 * jax.random.normal(arg_keys[7], (D,), jnp.float32), 0.099609375, 1.8984375).astype(jnp.bfloat16)
    expert_gate = centred(arg_keys[8], (EXPERTS, D, EXPERT_HIDDEN), D ** -0.5, 0.125, ((0, 8),))
    expert_up = centred(arg_keys[9], (EXPERTS, D, EXPERT_HIDDEN), D ** -0.5, 0.125, ((0, 8),))
    expert_down = draw_expert_down(jax.random.fold_in(arg_keys[17], 71), 0)
    shared_gate = centred(arg_keys[11], (D, SHARED_HIDDEN), D ** -0.5, 0.125)
    shared_up = centred(arg_keys[12], (D, SHARED_HIDDEN), D ** -0.5, 0.125)
    shared_down = draw_shared_down(jax.random.fold_in(arg_keys[17], 71), 0)
    post_gain = jnp.clip(1.0 + 0.18 * jax.random.normal(arg_keys[14], (D,), jnp.float32), 0.099609375, 1.8984375).astype(jnp.bfloat16)
    routes_keys = jax.random.split(jax.random.fold_in(arg_keys[15], 1), TOKENS // (TOK_DEV // N_TP))
    routes_turns = jax.random.permutation(jax.random.fold_in(arg_keys[15], 3), TOKENS // (TOK_DEV // N_TP))
    routes = jax.vmap(lambda own, number: assign_block(jax.random.fold_in(arg_keys[15], 2), own, number, TOK_DEV // N_TP, EXPERTS, TOPK, CAP, 2))(routes_keys, routes_turns).reshape((TOKENS, TOPK))
    route_weights = jnp.clip(0.1 + 0.9 * jax.random.uniform(arg_keys[16], (TOKENS, TOPK), jnp.float32) ** levels(arg_keys[16], (TOKENS, TOPK), ((0, 32),), -0.2, 0.2), 0.1, 1.0)
    return dict(x_in=x_in, gate_b=gate_b, gate_c=gate_c, conv_taps=conv_taps, out_proj=out_proj, mix_gain=mix_gain, resid=resid, pre_gain=pre_gain, expert_gate=expert_gate, expert_up=expert_up, expert_down=expert_down, shared_gate=shared_gate, shared_up=shared_up, shared_down=shared_down, post_gain=post_gain, routes=routes, route_weights=route_weights)


epsilon = 1e-06

def reference(x_in, gate_b, gate_c, conv_taps, out_proj, mix_gain, resid, pre_gain, expert_gate, expert_up, expert_down, shared_gate, shared_up, shared_down, post_gain, routes, route_weights):
    mixed_in = gate_c.astype(jnp.float32) * x_in.astype(jnp.float32)
    reach = CONV_WIDTH - 1
    padded = jnp.concatenate([jnp.zeros((reach, CONV_CH), jnp.float32), mixed_in], 0)
    taps = conv_taps.astype(jnp.float32)
    convolved = jnp.zeros((TOKENS, CONV_CH), jnp.float32)
    for index in range(CONV_WIDTH):
        convolved = convolved + taps[index][None, :] * padded[index:index + TOKENS]
    conv_out = (gate_b.astype(jnp.float32) * convolved).astype(jnp.bfloat16)
    projected = jnp.dot(conv_out, out_proj, preferred_element_type=jnp.float32)
    row_scale = lax.rsqrt(lax.optimization_barrier(jnp.mean(projected * projected, axis=1, keepdims=True)) + epsilon)
    resid1 = (resid.astype(jnp.float32) + projected * row_scale * mix_gain.astype(jnp.float32)).astype(jnp.bfloat16)
    wide_resid = resid1.astype(jnp.float32)
    normed = (wide_resid * lax.rsqrt(lax.optimization_barrier(jnp.mean(wide_resid * wide_resid, axis=1, keepdims=True)) + epsilon) * pre_gain.astype(jnp.float32)).astype(jnp.bfloat16)
    block_count = N_SP * N_TP
    quarter = TOK_DEV // N_TP
    flat_ids = routes.reshape(-1).astype(jnp.int32)
    onehot = (flat_ids[:, None] == jnp.arange(EXPERTS, dtype=jnp.int32)[None, :]).astype(jnp.int32)
    blocks = onehot.reshape(block_count, quarter * TOPK, EXPERTS)
    before = (jnp.cumsum(blocks, axis=1) - blocks).reshape(-1, EXPERTS)
    position = lax.optimization_barrier(jnp.sum(before * onehot, axis=1))
    source = jnp.arange(TOKENS * TOPK, dtype=jnp.int32) // (quarter * TOPK)
    slot_index = flat_ids * (block_count * CAP) + source * CAP + position
    dispatched = jnp.zeros((EXPERTS * block_count * CAP, D), jnp.bfloat16).at[slot_index].set(jnp.repeat(normed, TOPK, axis=0))

    def run_expert(operands):
        rows_in, w_gate, w_up, w_down = operands
        gate_h = jnp.dot(rows_in, w_gate, preferred_element_type=jnp.float32)
        up_h = jnp.dot(rows_in, w_up, preferred_element_type=jnp.float32)
        hidden = (jax.nn.silu(gate_h) * up_h).astype(jnp.bfloat16)
        return jnp.dot(hidden, w_down, preferred_element_type=jnp.float32).astype(jnp.bfloat16)
    expert_out = lax.map(run_expert, (dispatched.reshape(EXPERTS, block_count * CAP, D), expert_gate, expert_up, expert_down)).reshape(-1, D)
    picked = expert_out[slot_index].reshape(TOKENS, TOPK, D)
    routed = jnp.zeros((TOKENS, D), jnp.float32)
    for index in range(TOPK):
        routed = routed + route_weights[:, index:index + 1] * picked[:, index].astype(jnp.float32)
    shared_g = jnp.dot(normed, shared_gate, preferred_element_type=jnp.float32)
    shared_u = jnp.dot(normed, shared_up, preferred_element_type=jnp.float32)
    shared_hidden = (jax.nn.silu(shared_g) * shared_u).astype(jnp.bfloat16)
    shared_out = jnp.dot(shared_hidden, shared_down, preferred_element_type=jnp.float32)
    branch = routed + shared_out
    factor = lax.rsqrt(lax.optimization_barrier(jnp.mean(branch * branch, axis=1, keepdims=True)) + epsilon)
    return (wide_resid + branch * factor * post_gain.astype(jnp.float32)).astype(jnp.bfloat16)
```

```python
import functools

import jax
import jax.numpy as jnp
from jax import lax
from jax.experimental import pallas as pl
from jax.experimental.pallas import tpu as pltpu

P = jax.sharding.PartitionSpec
MESH = pl.DeviceIdType.MESH
epsilon = 1e-06
PIECES = 4
HALVES = 2


def moe_kernel(
    line,
    normed_ref,
    resid_ref,
    routes_ref,
    weights_ref,
    post_ref,
    eg_ref,
    eu_ref,
    ed_ref,
    sg_ref,
    su_ref,
    sd_ref,
    out_ref,
    w_gate,
    w_up,
    w_down,
    s_gate,
    s_up,
    s_down,
    blocks,
    sums,
    shared,
    from_low,
    from_high,
    outgoing,
    shares,
    hidden,
    load_sem,
    wx_send,
    wx_recv,
    wn_send,
    wn_recv,
    wf_send,
    wf_recv,
    wr_send,
    wr_recv,
    t_send,
    t_recv,
    gu_send,
    gu_recv,
    gd_send,
    gd_recv,
    ru_send,
    ru_recv,
    rd_send,
    rd_recv,
):
    sp = lax.axis_index("sp")
    tp = lax.axis_index("tp")
    sp_size = lax.axis_size("sp")
    tp_size = lax.axis_size("tp")
    z = sp // 2
    x = sp % 2
    last = line - 1
    mate = z * 2 + 1 - x
    near = (tp // 2) * 2 + 1 - tp % 2
    far = (tp + 2) % tp_size
    near_far = (near + 2) % tp_size
    rows, width = normed_ref.shape
    step_rows = rows // PIECES
    hid = w_gate.shape[2]
    shared_hid = s_gate.shape[1]

    barrier = pltpu.get_barrier_semaphore()
    for k in range(1, sp_size):
        pl.semaphore_signal(barrier, inc=1, device_id=((sp + k) % sp_size, tp), device_id_type=MESH)
    for k in range(1, tp_size):
        pl.semaphore_signal(barrier, inc=1, device_id=(sp, (tp + k) % tp_size), device_id_type=MESH)

    loads = [
        pltpu.make_async_copy(src, dst, load_sem.at[n])
        for n, (src, dst) in enumerate(
            (
                (eg_ref.at[0], w_gate.at[0]),
                (eu_ref.at[0], w_up.at[0]),
                (ed_ref.at[0], w_down.at[0]),
                (sg_ref, s_gate),
                (su_ref, s_up),
                (sd_ref, s_down),
            )
        )
    ]
    for load in loads:
        load.start()
    pl.semaphore_wait(barrier, sp_size - 1 + tp_size - 1)

    pieces = []
    for ref, held in ((eg_ref, w_gate), (eu_ref, w_up), (ed_ref, w_down)):
        size = ref.shape[1] // tp_size // HALVES
        for h in range(HALVES):
            pieces.append((ref, held, size, h))

    def span(owner, n):
        _, _, size, h = pieces[n]
        return pl.ds(pl.multiple_of((owner * HALVES + h) * size, size), size)

    def hop(n, owner, target, send, recv, first=False):
        ref, held, _, _ = pieces[n]
        where = span(owner, n)
        return pltpu.make_async_remote_copy(
            src_ref=ref.at[0, where] if first else held.at[1, where],
            dst_ref=held.at[1, where],
            send_sem=send.at[n],
            recv_sem=recv.at[n],
            device_id=target,
            device_id_type=MESH,
        )

    def x_hop(n):
        return hop(n, tp, (mate, tp), wx_send, wx_recv, True)

    def near_hop(n, owner):
        return hop(n, owner, (sp, near), wn_send, wn_recv)

    def far_hop(n, owner):
        return hop(n, owner, (sp, far), wf_send, wf_recv)

    def relay_hop(n, owner):
        return hop(n, owner, (sp, near), wr_send, wr_recv)

    count = len(pieces)

    def line_copy(source, landing, b, c, up, send, recv):
        part = pl.ds(pl.multiple_of(c * step_rows, step_rows), step_rows)
        return pltpu.make_async_remote_copy(
            src_ref=source.at[b, part],
            dst_ref=landing.at[b, part],
            send_sem=send.at[b, c],
            recv_sem=recv.at[b, c],
            device_id=((z + (1 if up else -1)) * 2 + x, tp),
            device_id_type=MESH,
        )

    def go_up(b, c):
        return line_copy(blocks, blocks, b, c, True, gu_send, gu_recv)

    def go_down(b, c):
        return line_copy(blocks, blocks, b, c, False, gd_send, gd_recv)

    def back_up(b, c):
        return line_copy(outgoing, from_low, b, c, True, ru_send, ru_recv)

    def back_down(b, c):
        return line_copy(outgoing, from_high, b, c, False, rd_send, rd_recv)

    def share_copy(k, source):
        return pltpu.make_async_remote_copy(
            src_ref=shares.at[source],
            dst_ref=shares.at[source],
            send_sem=t_send.at[k],
            recv_sem=t_recv.at[source],
            device_id=(((z + k) % line) * 2 + x, tp),
            device_id_type=MESH,
        )

    lanes = lax.broadcasted_iota(jnp.int32, (rows, shares.shape[2]), 1)
    table = jnp.zeros((rows, shares.shape[2]), jnp.float32)
    for k in range(routes_ref.shape[1]):
        table += jnp.where(lanes == routes_ref[:, k : k + 1], weights_ref[:, k : k + 1], 0.0)
    shares[z] = table
    blocks[z] = normed_ref[...]
    sums[...] = jnp.zeros_like(sums)
    for c in range(PIECES):

        @pl.when(z < last)
        def _():
            go_up(z, c).start()

        @pl.when(z > 0)
        def _():
            go_down(z, c).start()

    for n in range(count):
        x_hop(n).start()
    for k in range(1, line):
        share_copy(k, z).start()

    def apply(b, i):
        expert = z * 2 + x + i * (1 - 2 * x)

        @pl.loop(0, hid // 256)
        def _(j):
            cols = pl.ds(pl.multiple_of(j * 256, 256), 256)
            gate = jnp.dot(blocks[b], w_gate[i, :, cols], preferred_element_type=jnp.float32)
            up = jnp.dot(blocks[b], w_up[i, :, cols], preferred_element_type=jnp.float32)
            hidden[:, cols] = (jax.nn.silu(gate) * up).astype(jnp.bfloat16)

        share = jnp.sum(jnp.where(lanes == expert, shares[b], 0.0), axis=1, keepdims=True)

        @pl.loop(0, width // 512)
        def _(j):
            cols = pl.ds(pl.multiple_of(j * 512, 512), 512)
            made = jnp.dot(hidden[...], w_down[i, :, cols], preferred_element_type=jnp.float32)
            made = made.astype(jnp.bfloat16).astype(jnp.float32)
            sums[b, :, cols] += jnp.where(share > 0.0, share * made, 0.0)

    def receive(t):
        @pl.loop(0, PIECES)
        def _(c):
            @pl.when(z - t >= 0)
            def _():
                go_up(z - t, c).wait_recv()

                @pl.when(z < last)
                def _():
                    go_up(z - t, c).start()

            @pl.when(z + t <= last)
            def _():
                go_down(z + t, c).wait_recv()

                @pl.when(z > 0)
                def _():
                    go_down(z + t, c).start()

    def apply_pair(t, i):
        @pl.loop(0, 2)
        def _(side):
            b = z - t + side * 2 * t

            @pl.when((b >= 0) & (b <= last))
            def _():
                apply(b, i)

    def give_back(t):
        b_up = t - z
        b_down = 2 * last - z - t

        @pl.loop(0, PIECES)
        def _(c):
            part = pl.ds(pl.multiple_of(c * step_rows, step_rows), step_rows)

            @pl.when((b_up > z) & (b_up <= last))
            def _():
                @pl.when(z > 0)
                def _():
                    back_up(b_up, c).wait_recv()
                    sums[b_up, part] += from_low[b_up, part].astype(jnp.float32)

                outgoing[b_up, part] = sums[b_up, part].astype(jnp.bfloat16)
                back_up(b_up, c).start()

            @pl.when((b_down < z) & (b_down >= 0))
            def _():
                @pl.when(z < last)
                def _():
                    back_down(b_down, c).wait_recv()
                    sums[b_down, part] += from_high[b_down, part].astype(jnp.float32)

                outgoing[b_down, part] = sums[b_down, part].astype(jnp.bfloat16)
                back_down(b_down, c).start()

    for load in loads[:3]:
        load.wait()
    apply(z, 0)
    for load in loads[3:]:
        load.wait()
    s_g = jnp.dot(blocks[z], s_gate[...], preferred_element_type=jnp.float32)
    s_u = jnp.dot(blocks[z], s_up[...], preferred_element_type=jnp.float32)
    s_h = (jax.nn.silu(s_g) * s_u).astype(jnp.bfloat16)
    hidden[:, :shared_hid] = s_h

    @pl.loop(0, width // 512)
    def _(j):
        cols = pl.ds(pl.multiple_of(j * 512, 512), 512)
        shared[:, cols] = jnp.dot(
            hidden[:, :shared_hid], s_down[:, cols], preferred_element_type=jnp.float32
        )

    for n in range(count):
        x_hop(n).wait_recv()
        far_hop(n, tp).start()
        near_hop(n, tp).start()
    receive(1)
    for k in range(1, line):
        share_copy(k, (z + k) % line).wait_recv()
    apply_pair(1, 0)
    for n in range(count):
        far_hop(n, far).wait_recv()
        relay_hop(n, far).start()
    receive(2)
    for n in range(count):
        near_hop(n, near).wait_recv()
        relay_hop(n, near_far).wait_recv()
    apply_pair(1, 1)
    give_back(1)

    @pl.loop(2, line)
    def _(t):
        @pl.when(t > 2)
        def _():
            receive(t)

        apply_pair(t, 0)
        apply_pair(t, 1)
        give_back(t)

    apply(z, 1)

    @pl.loop(line, 2 * line - 2)
    def _(t):
        give_back(t)

    @pl.loop(0, PIECES)
    def _(c):
        part = pl.ds(pl.multiple_of(c * step_rows, step_rows), step_rows)

        @pl.when(z > 0)
        def _():
            back_up(z, c).wait_recv()
            sums[z, part] += from_low[z, part].astype(jnp.float32)

        @pl.when(z < last)
        def _():
            back_down(z, c).wait_recv()
            sums[z, part] += from_high[z, part].astype(jnp.float32)

        branch = sums[z, part] + shared[part]
        factor = lax.rsqrt(jnp.mean(branch * branch, axis=1, keepdims=True) + epsilon)
        out_ref[part] = (
            resid_ref[part].astype(jnp.float32)
            + branch * factor * post_ref[...].astype(jnp.float32)
        ).astype(jnp.bfloat16)

    for n in range(count):
        x_hop(n).wait_send()
        near_hop(n, tp).wait_send()
        far_hop(n, tp).wait_send()
        relay_hop(n, far).wait_send()
    for k in range(1, line):
        share_copy(k, z).wait_send()

    @pl.loop(0, PIECES)
    def _(c):
        @pl.loop(0, line)
        def _(b):
            @pl.when((b <= z) & (z < last))
            def _():
                go_up(b, c).wait_send()

            @pl.when((b >= z) & (z > 0))
            def _():
                go_down(b, c).wait_send()

            @pl.when(b > z)
            def _():
                back_up(b, c).wait_send()

            @pl.when(b < z)
            def _():
                back_down(b, c).wait_send()


def routed_and_shared(
    normed, resid1, routes, route_weights, post_gain, expert_gate, expert_up, expert_down,
    shared_gate, shared_up, shared_down,
):
    experts = lax.axis_size("sp")
    line = experts // 2
    rows, width = normed.shape
    hid = expert_gate.shape[2]
    shared_hid = shared_gate.shape[1]
    dma = pltpu.SemaphoreType.DMA
    count = 3 * HALVES
    bf, f32 = jnp.bfloat16, jnp.float32
    vmem = pl.BlockSpec(memory_space=pltpu.VMEM)
    anywhere = pl.BlockSpec(memory_space=pltpu.HBM)
    lanes = 128 * (-(-experts // 128))
    return pl.pallas_call(
        functools.partial(moe_kernel, line),
        out_shape=jax.ShapeDtypeStruct((rows, width), bf),
        in_specs=[vmem] * 5 + [anywhere] * 6,
        out_specs=vmem,
        scratch_shapes=[
            pltpu.VMEM((2, width, hid), bf),
            pltpu.VMEM((2, width, hid), bf),
            pltpu.VMEM((2, hid, width), bf),
            pltpu.VMEM((width, shared_hid), bf),
            pltpu.VMEM((width, shared_hid), bf),
            pltpu.VMEM((shared_hid, width), bf),
            pltpu.VMEM((line, rows, width), bf),
            pltpu.VMEM((line, rows, width), f32),
            pltpu.VMEM((rows, width), f32),
            pltpu.VMEM((line, rows, width), bf),
            pltpu.VMEM((line, rows, width), bf),
            pltpu.VMEM((line, rows, width), bf),
            pltpu.VMEM((line, rows, lanes), f32),
            pltpu.VMEM((rows, max(hid, shared_hid)), bf),
            dma((6,)),
        ]
        + [dma((count,))] * 8
        + [dma((line,))] * 2
        + [dma((line, PIECES))] * 8,
        compiler_params=pltpu.CompilerParams(
            collective_id=0, has_side_effects=True, vmem_limit_bytes=60 * 1024 * 1024
        ),
    )(
        normed, resid1, routes, route_weights, post_gain.reshape(1, width),
        expert_gate, expert_up, expert_down, shared_gate, shared_up, shared_down,
    )


def passed_along(shard, axis, by):
    size = lax.axis_size(axis)
    pairs = [(i, i + by) for i in range(size) if 0 <= i + by < size]
    return lax.ppermute(shard, axis, pairs)


def body(
    x_in,
    gate_b,
    gate_c,
    conv_taps,
    out_proj,
    mix_gain,
    resid,
    pre_gain,
    expert_gate,
    expert_up,
    expert_down,
    shared_gate,
    shared_up,
    shared_down,
    post_gain,
    routes,
    route_weights,
):
    row_count = x_in.shape[0]
    channels = x_in.shape[1]
    reach = conv_taps.shape[0] - 1
    edge_rows = jnp.concatenate([x_in[row_count - reach :], gate_c[row_count - reach :]], 1)
    arrived_edge = passed_along(edge_rows, "sp", 1)
    inputs = jnp.concatenate([arrived_edge[:, :channels], x_in], 0).astype(jnp.float32)
    gate_rows = jnp.concatenate([arrived_edge[:, channels:], gate_c], 0).astype(jnp.float32)
    mixed_in = inputs * gate_rows
    taps = conv_taps.astype(jnp.float32)
    convolved = jnp.zeros((row_count, channels), jnp.float32)
    for index in range(reach + 1):
        convolved = convolved + taps[index][None, :] * mixed_in[index : index + row_count]
    conv_out = (gate_b.astype(jnp.float32) * convolved).astype(jnp.bfloat16)
    width_all = out_proj.shape[1]
    full_rows = lax.all_to_all(conv_out, "tp", split_axis=0, concat_axis=1, tiled=True)
    projected = jnp.dot(
        full_rows,
        lax.all_gather(out_proj, "tp", axis=0, tiled=True),
        preferred_element_type=jnp.float32,
    )
    row_scale = lax.rsqrt(jnp.mean(projected * projected, axis=1, keepdims=True) + epsilon)
    resid1 = (
        resid.astype(jnp.float32) + projected * row_scale * mix_gain.astype(jnp.float32)
    ).astype(jnp.bfloat16)
    wide_resid = resid1.astype(jnp.float32)
    normed = (
        wide_resid
        * lax.rsqrt(jnp.mean(wide_resid * wide_resid, axis=1, keepdims=True) + epsilon)
        * pre_gain.astype(jnp.float32)
    ).astype(jnp.bfloat16)
    experts = lax.axis_size("sp")
    local_rows = resid.shape[0]
    top_count = routes.shape[1]
    capacity = 3 * local_rows * top_count // (2 * experts)
    if 2 * capacity > local_rows and experts % 2 == 0 and lax.axis_size("tp") == 2 * 2:
        return routed_and_shared(
            normed, resid1, routes, route_weights, post_gain, expert_gate, expert_up, expert_down,
            shared_gate, shared_up, shared_down,
        )
    flat_ids = routes.reshape(-1)
    onehot = (flat_ids[:, None] == jnp.arange(experts, dtype=jnp.int32)[None, :]).astype(jnp.int32)
    before = jnp.cumsum(onehot, axis=0) - onehot
    position = jnp.sum(before * onehot, axis=1)
    slot_index = flat_ids * capacity + position
    outgoing = (
        jnp.zeros((experts * capacity, width_all), jnp.bfloat16)
        .at[slot_index]
        .set(jnp.repeat(normed, top_count, axis=0))
    )
    received = lax.all_to_all(
        outgoing.reshape(experts, capacity, width_all),
        "sp",
        split_axis=0,
        concat_axis=0,
        tiled=True,
    )
    arrived = received.reshape(experts * capacity, width_all)
    gate_h = jnp.dot(arrived, expert_gate[0], preferred_element_type=jnp.float32)
    up_h = jnp.dot(arrived, expert_up[0], preferred_element_type=jnp.float32)
    hidden = (jax.nn.silu(gate_h) * up_h).astype(jnp.bfloat16)
    expert_out = jnp.dot(hidden, expert_down[0], preferred_element_type=jnp.float32).astype(
        jnp.bfloat16
    )
    returned = lax.all_to_all(
        expert_out.reshape(experts, capacity, width_all),
        "sp",
        split_axis=0,
        concat_axis=0,
        tiled=True,
    )
    returned = returned.reshape(experts * capacity, width_all)
    picked = returned[slot_index].astype(jnp.float32).reshape(local_rows, top_count, width_all)
    routed = jnp.einsum("tk,tkd->td", route_weights, picked)
    shared_g = jnp.dot(normed, shared_gate, preferred_element_type=jnp.float32)
    shared_u = jnp.dot(normed, shared_up, preferred_element_type=jnp.float32)
    shared_hidden = (jax.nn.silu(shared_g) * shared_u).astype(jnp.bfloat16)
    shared_out = jnp.dot(shared_hidden, shared_down, preferred_element_type=jnp.float32)
    branch = routed + shared_out
    factor = lax.rsqrt(jnp.mean(branch * branch, axis=1, keepdims=True) + epsilon)
    return (wide_resid + branch * factor * post_gain.astype(jnp.float32)[None, :]).astype(
        jnp.bfloat16
    )


def solution(mesh):
    return jax.shard_map(
        body,
        mesh=mesh,
        in_specs=(
            P("sp", "tp"),
            P("sp", "tp"),
            P("sp", "tp"),
            P(None, "tp"),
            P("tp", None),
            P(),
            P(("sp", "tp"), None),
            P(),
            P("sp", None, None),
            P("sp", None, None),
            P("sp", None, None),
            P(),
            P(),
            P(),
            P(),
            P(("sp", "tp"), None),
            P(("sp", "tp"), None),
        ),
        out_specs=P(("sp", "tp"), None),
        check_vma=False,
    )
```

```python
import functools

import jax
import jax.numpy as jnp
from jax import lax
from jax.experimental import pallas as pl
from jax.experimental.pallas import tpu as pltpu

P = jax.sharding.PartitionSpec
MESH = pl.DeviceIdType.MESH
epsilon = 1e-06
PIECES = 4
HALVES = 2


def layer_kernel(
    line,
    x_ref,
    gate_b_ref,
    gate_c_ref,
    taps_ref,
    resid_ref,
    gains_ref,
    routes_ref,
    weights_ref,
    proj_ref,
    eg_ref,
    eu_ref,
    ed_ref,
    sg_ref,
    su_ref,
    sd_ref,
    out_ref,
    edge_x,
    edge_c,
    mixed,
    conv,
    conv_near,
    proj,
    part_out,
    part_in,
    projected,
    resid1,
    w_gate,
    w_up,
    w_down,
    s_gate,
    s_up,
    s_down,
    blocks,
    sums,
    shared,
    from_low,
    from_high,
    outgoing,
    shares,
    hidden,
    load_sem,
    e_send,
    e_recv,
    p_send,
    p_recv,
    c_send,
    c_recv,
    f_send,
    f_recv,
    wx_send,
    wx_recv,
    wn_send,
    wn_recv,
    wf_send,
    wf_recv,
    wr_send,
    wr_recv,
    t_send,
    t_recv,
    gu_send,
    gu_recv,
    gd_send,
    gd_recv,
    ru_send,
    ru_recv,
    rd_send,
    rd_recv,
):
    sp = lax.axis_index("sp")
    tp = lax.axis_index("tp")
    sp_size = lax.axis_size("sp")
    tp_size = lax.axis_size("tp")
    z = sp // 2
    x = sp % 2
    last = line - 1
    mate = z * 2 + 1 - x
    near = (tp // 2) * 2 + 1 - tp % 2
    far = (tp + 2) % tp_size
    near_far = (near + 2) % tp_size
    rows, width = resid_ref.shape
    step_rows = rows // PIECES
    hid = w_gate.shape[2]
    shared_hid = s_gate.shape[1]

    barrier = pltpu.get_barrier_semaphore()
    for k in range(1, sp_size):
        pl.semaphore_signal(barrier, inc=1, device_id=((sp + k) % sp_size, tp), device_id_type=MESH)
    for k in range(1, tp_size):
        pl.semaphore_signal(barrier, inc=1, device_id=(sp, (tp + k) % tp_size), device_id_type=MESH)

    loads = [
        pltpu.make_async_copy(src, dst, load_sem.at[n])
        for n, (src, dst) in enumerate(
            (
                (eg_ref.at[0], w_gate.at[0]),
                (eu_ref.at[0], w_up.at[0]),
                (ed_ref.at[0], w_down.at[0]),
                (sg_ref, s_gate),
                (su_ref, s_up),
                (sd_ref, s_down),
                (proj_ref, proj.at[0]),
            )
        )
    ]
    loads[-1].start()
    for load in loads[:-1]:
        load.start()

    all_rows, channels = x_ref.shape
    reach = taps_ref.shape[0] - 1
    pad = edge_x.shape[0]
    mixed[pad:] = x_ref[...].astype(jnp.float32) * gate_c_ref[...].astype(jnp.float32)

    def edge_copy(n):
        source, landing = ((x_ref, edge_x), (gate_c_ref, edge_c))[n]
        return pltpu.make_async_remote_copy(
            src_ref=source.at[pl.ds(all_rows - pad, pad)],
            dst_ref=landing,
            send_sem=e_send.at[n],
            recv_sem=e_recv.at[n],
            device_id=((sp + 1) % sp_size, tp),
            device_id_type=MESH,
        )

    proj_copy = pltpu.make_async_remote_copy(
        src_ref=proj_ref,
        dst_ref=proj.at[1],
        send_sem=p_send.at[0],
        recv_sem=p_recv.at[0],
        device_id=(sp, near),
        device_id_type=MESH,
    )

    def block_rows(owner):
        return pl.ds(pl.multiple_of(owner * rows, rows), rows)

    def conv_copy(n):
        return pltpu.make_async_remote_copy(
            src_ref=conv.at[block_rows((near, near_far)[n])],
            dst_ref=conv_near.at[n],
            send_sem=c_send.at[n],
            recv_sem=c_recv.at[n],
            device_id=(sp, near),
            device_id_type=MESH,
        )

    part_cols = width // PIECES

    def part_copy(j):
        cols = pl.ds(pl.multiple_of(j * part_cols, part_cols), part_cols)
        return pltpu.make_async_remote_copy(
            src_ref=part_out.at[:, cols],
            dst_ref=part_in.at[:, cols],
            send_sem=f_send.at[j],
            recv_sem=f_recv.at[j],
            device_id=(sp, far),
            device_id_type=MESH,
        )

    pl.semaphore_wait(barrier, sp_size - 1 + tp_size - 1)

    @pl.when(sp < sp_size - 1)
    def _():
        edge_copy(0).start()
        edge_copy(1).start()

    proj_copy.start()

    pieces = []
    for ref, held in ((eg_ref, w_gate), (eu_ref, w_up), (ed_ref, w_down)):
        size = ref.shape[1] // tp_size // HALVES
        for h in range(HALVES):
            pieces.append((ref, held, size, h))

    def span(owner, n):
        _, _, size, h = pieces[n]
        return pl.ds(pl.multiple_of((owner * HALVES + h) * size, size), size)

    def hop(n, owner, target, send, recv, first=False):
        ref, held, _, _ = pieces[n]
        where = span(owner, n)
        return pltpu.make_async_remote_copy(
            src_ref=ref.at[0, where] if first else held.at[1, where],
            dst_ref=held.at[1, where],
            send_sem=send.at[n],
            recv_sem=recv.at[n],
            device_id=target,
            device_id_type=MESH,
        )

    def x_hop(n):
        return hop(n, tp, (mate, tp), wx_send, wx_recv, True)

    def near_hop(n, owner):
        return hop(n, owner, (sp, near), wn_send, wn_recv)

    def far_hop(n, owner):
        return hop(n, owner, (sp, far), wf_send, wf_recv)

    def relay_hop(n, owner):
        return hop(n, owner, (sp, near), wr_send, wr_recv)

    count = len(pieces)

    def line_copy(source, landing, b, c, up, send, recv):
        part = pl.ds(pl.multiple_of(c * step_rows, step_rows), step_rows)
        return pltpu.make_async_remote_copy(
            src_ref=source.at[b, part],
            dst_ref=landing.at[b, part],
            send_sem=send.at[b, c],
            recv_sem=recv.at[b, c],
            device_id=((z + (1 if up else -1)) * 2 + x, tp),
            device_id_type=MESH,
        )

    def go_up(b, c):
        return line_copy(blocks, blocks, b, c, True, gu_send, gu_recv)

    def go_down(b, c):
        return line_copy(blocks, blocks, b, c, False, gd_send, gd_recv)

    def back_up(b, c):
        return line_copy(outgoing, from_low, b, c, True, ru_send, ru_recv)

    def back_down(b, c):
        return line_copy(outgoing, from_high, b, c, False, rd_send, rd_recv)

    def share_copy(k, source):
        return pltpu.make_async_remote_copy(
            src_ref=shares.at[source],
            dst_ref=shares.at[source],
            send_sem=t_send.at[k],
            recv_sem=t_recv.at[source],
            device_id=(((z + k) % line) * 2 + x, tp),
            device_id_type=MESH,
        )

    for n in range(count):
        x_hop(n).start()

    lanes = lax.broadcasted_iota(jnp.int32, (rows, shares.shape[2]), 1)
    table = jnp.zeros((rows, shares.shape[2]), jnp.float32)
    for k in range(routes_ref.shape[1]):
        table += jnp.where(lanes == routes_ref[:, k : k + 1], weights_ref[:, k : k + 1], 0.0)
    shares[z] = table

    @pl.when(sp > 0)
    def _():
        edge_copy(0).wait_recv()
        edge_copy(1).wait_recv()
        mixed[:pad] = edge_x[...].astype(jnp.float32) * edge_c[...].astype(jnp.float32)

    @pl.when(sp == 0)
    def _():
        mixed[:pad] = jnp.zeros((pad, channels), jnp.float32)

    convolved = jnp.zeros((all_rows, channels), jnp.float32)
    for k in range(reach + 1):
        begin = pad - reach + k
        convolved += taps_ref[k : k + 1].astype(jnp.float32) * mixed[begin : begin + all_rows]
    conv[...] = (gate_b_ref[...].astype(jnp.float32) * convolved).astype(jnp.bfloat16)
    conv_copy(1).start()
    conv_copy(0).start()
    for k in range(1, line):
        share_copy(k, z).start()
    loads[-1].wait()
    proj_copy.wait_recv()

    def project(n, owner, cols):
        return jnp.dot(
            conv[block_rows(owner)], proj[0, :, cols], preferred_element_type=jnp.float32
        ) + jnp.dot(conv_near[n], proj[1, :, cols], preferred_element_type=jnp.float32)

    conv_copy(1).wait_recv()

    @pl.loop(0, PIECES)
    def _(j):
        cols = pl.ds(pl.multiple_of(j * part_cols, part_cols), part_cols)
        part_out[:, cols] = project(1, far, cols).astype(jnp.bfloat16)
        part_copy(j).start()

    conv_copy(0).wait_recv()

    @pl.loop(0, PIECES)
    def _(j):
        cols = pl.ds(pl.multiple_of(j * part_cols, part_cols), part_cols)
        projected[:, cols] = project(0, tp, cols)

    sums[...] = jnp.zeros_like(sums)

    def spread(n):
        x_hop(n).wait_recv()
        far_hop(n, tp).start()
        near_hop(n, tp).start()

    for n in range(count // 2):
        spread(n)

    @pl.loop(0, PIECES)
    def _(j):
        cols = pl.ds(pl.multiple_of(j * part_cols, part_cols), part_cols)
        part_copy(j).wait_recv()
        projected[:, cols] += part_in[:, cols].astype(jnp.float32)

    def send_block(c):
        @pl.when(z < last)
        def _():
            go_up(z, c).start()

        @pl.when(z > 0)
        def _():
            go_down(z, c).start()

    for c in range(PIECES):
        part = pl.ds(c * step_rows, step_rows)
        block = projected[part]
        scale = lax.rsqrt(jnp.mean(block * block, axis=1, keepdims=True) + epsilon)
        mid = (
            resid_ref[part].astype(jnp.float32)
            + block * scale * gains_ref[0:1].astype(jnp.float32)
        ).astype(jnp.bfloat16)
        resid1[part] = mid
        wide = mid.astype(jnp.float32)
        normal = lax.rsqrt(jnp.mean(wide * wide, axis=1, keepdims=True) + epsilon)
        blocks[z, part] = (wide * normal * gains_ref[1:2].astype(jnp.float32)).astype(jnp.bfloat16)
        if c > 0:
            send_block(c - 1)
    send_block(PIECES - 1)

    def apply(b, i):
        expert = z * 2 + x + i * (1 - 2 * x)

        @pl.loop(0, hid // 256)
        def _(j):
            cols = pl.ds(pl.multiple_of(j * 256, 256), 256)
            gate = jnp.dot(blocks[b], w_gate[i, :, cols], preferred_element_type=jnp.float32)
            up = jnp.dot(blocks[b], w_up[i, :, cols], preferred_element_type=jnp.float32)
            hidden[:, cols] = (jax.nn.silu(gate) * up).astype(jnp.bfloat16)

        share = jnp.sum(jnp.where(lanes == expert, shares[b], 0.0), axis=1, keepdims=True)

        @pl.loop(0, width // 512)
        def _(j):
            cols = pl.ds(pl.multiple_of(j * 512, 512), 512)
            made = jnp.dot(hidden[...], w_down[i, :, cols], preferred_element_type=jnp.float32)
            made = made.astype(jnp.bfloat16).astype(jnp.float32)
            sums[b, :, cols] += jnp.where(share > 0.0, share * made, 0.0)

    def receive(t):
        @pl.loop(0, PIECES)
        def _(c):
            @pl.when(z - t >= 0)
            def _():
                go_up(z - t, c).wait_recv()

                @pl.when(z < last)
                def _():
                    go_up(z - t, c).start()

            @pl.when(z + t <= last)
            def _():
                go_down(z + t, c).wait_recv()

                @pl.when(z > 0)
                def _():
                    go_down(z + t, c).start()

    def apply_pair(t, i):
        @pl.loop(0, 2)
        def _(side):
            b = z - t + side * 2 * t

            @pl.when((b >= 0) & (b <= last))
            def _():
                apply(b, i)

    def give_back(t):
        b_up = t - z
        b_down = 2 * last - z - t

        @pl.loop(0, PIECES)
        def _(c):
            part = pl.ds(pl.multiple_of(c * step_rows, step_rows), step_rows)

            @pl.when((b_up > z) & (b_up <= last))
            def _():
                @pl.when(z > 0)
                def _():
                    back_up(b_up, c).wait_recv()
                    sums[b_up, part] += from_low[b_up, part].astype(jnp.float32)

                outgoing[b_up, part] = sums[b_up, part].astype(jnp.bfloat16)
                back_up(b_up, c).start()

            @pl.when((b_down < z) & (b_down >= 0))
            def _():
                @pl.when(z < last)
                def _():
                    back_down(b_down, c).wait_recv()
                    sums[b_down, part] += from_high[b_down, part].astype(jnp.float32)

                outgoing[b_down, part] = sums[b_down, part].astype(jnp.bfloat16)
                back_down(b_down, c).start()

    for load in loads[:3]:
        load.wait()
    apply(z, 0)
    for load in loads[3:-1]:
        load.wait()
    s_g = jnp.dot(blocks[z], s_gate[...], preferred_element_type=jnp.float32)
    s_u = jnp.dot(blocks[z], s_up[...], preferred_element_type=jnp.float32)
    s_h = (jax.nn.silu(s_g) * s_u).astype(jnp.bfloat16)
    hidden[:, :shared_hid] = s_h

    @pl.loop(0, width // 512)
    def _(j):
        cols = pl.ds(pl.multiple_of(j * 512, 512), 512)
        shared[:, cols] = jnp.dot(
            hidden[:, :shared_hid], s_down[:, cols], preferred_element_type=jnp.float32
        )

    for n in range(count // 2, count):
        spread(n)
    receive(1)
    for k in range(1, line):
        share_copy(k, (z + k) % line).wait_recv()
    apply_pair(1, 0)

    def relay(n):
        far_hop(n, far).wait_recv()
        relay_hop(n, far).start()

    for n in range(2 * count // 3):
        relay(n)
    for t in range(2, last):
        receive(t)
        apply_pair(t, 0)
    for n in range(2 * count // 3, count):
        relay(n)
    for n in range(count):
        near_hop(n, near).wait_recv()
        relay_hop(n, near_far).wait_recv()

    @pl.loop(1, last)
    def _(t):
        apply_pair(t, 1)
        give_back(t)

    receive(last)
    apply_pair(last, 0)
    apply_pair(last, 1)
    give_back(last)
    apply(z, 1)

    @pl.loop(line, 2 * line - 2)
    def _(t):
        give_back(t)

    @pl.loop(0, PIECES)
    def _(c):
        part = pl.ds(pl.multiple_of(c * step_rows, step_rows), step_rows)

        @pl.when(z > 0)
        def _():
            back_up(z, c).wait_recv()
            sums[z, part] += from_low[z, part].astype(jnp.float32)

        @pl.when(z < last)
        def _():
            back_down(z, c).wait_recv()
            sums[z, part] += from_high[z, part].astype(jnp.float32)

        branch = sums[z, part] + shared[part]
        factor = lax.rsqrt(jnp.mean(branch * branch, axis=1, keepdims=True) + epsilon)
        out_ref[part] = (
            resid1[part].astype(jnp.float32)
            + branch * factor * gains_ref[2:3].astype(jnp.float32)
        ).astype(jnp.bfloat16)

    @pl.when(sp < sp_size - 1)
    def _():
        edge_copy(0).wait_send()
        edge_copy(1).wait_send()

    proj_copy.wait_send()
    conv_copy(0).wait_send()
    conv_copy(1).wait_send()
    for j in range(PIECES):
        part_copy(j).wait_send()
    for n in range(count):
        x_hop(n).wait_send()
        near_hop(n, tp).wait_send()
        far_hop(n, tp).wait_send()
        relay_hop(n, far).wait_send()
    for k in range(1, line):
        share_copy(k, z).wait_send()

    @pl.loop(0, PIECES)
    def _(c):
        @pl.loop(0, line)
        def _(b):
            @pl.when((b <= z) & (z < last))
            def _():
                go_up(b, c).wait_send()

            @pl.when((b >= z) & (z > 0))
            def _():
                go_down(b, c).wait_send()

            @pl.when(b > z)
            def _():
                back_up(b, c).wait_send()

            @pl.when(b < z)
            def _():
                back_down(b, c).wait_send()


def fused_layer(
    x_in, gate_b, gate_c, conv_taps, out_proj, mix_gain, resid, pre_gain, expert_gate, expert_up,
    expert_down, shared_gate, shared_up, shared_down, post_gain, routes, route_weights,
):
    experts = lax.axis_size("sp")
    line = experts // 2
    all_rows, channels = x_in.shape
    rows, width = resid.shape
    hid = expert_gate.shape[2]
    shared_hid = shared_gate.shape[1]
    dma = pltpu.SemaphoreType.DMA
    count = 3 * HALVES
    bf, f32 = jnp.bfloat16, jnp.float32
    vmem = pl.BlockSpec(memory_space=pltpu.VMEM)
    hbm = pl.BlockSpec(memory_space=pltpu.HBM)
    lanes = 128 * (-(-experts // 128))
    pad = 16 * (-(-(conv_taps.shape[0] - 1) // 16))
    return pl.pallas_call(
        functools.partial(layer_kernel, line),
        out_shape=jax.ShapeDtypeStruct((rows, width), bf),
        in_specs=[vmem] * 8 + [hbm] * 7,
        out_specs=vmem,
        scratch_shapes=[
            pltpu.VMEM((pad, channels), bf),
            pltpu.VMEM((pad, channels), bf),
            pltpu.VMEM((pad + all_rows, channels), f32),
            pltpu.VMEM((all_rows, channels), bf),
            pltpu.VMEM((2, rows, channels), bf),
            pltpu.VMEM((2, channels, width), bf),
            pltpu.VMEM((rows, width), bf),
            pltpu.VMEM((rows, width), bf),
            pltpu.VMEM((rows, width), f32),
            pltpu.VMEM((rows, width), bf),
            pltpu.VMEM((2, width, hid), bf),
            pltpu.VMEM((2, width, hid), bf),
            pltpu.VMEM((2, hid, width), bf),
            pltpu.VMEM((width, shared_hid), bf),
            pltpu.VMEM((width, shared_hid), bf),
            pltpu.VMEM((shared_hid, width), bf),
            pltpu.VMEM((line, rows, width), bf),
            pltpu.VMEM((line, rows, width), f32),
            pltpu.VMEM((rows, width), f32),
            pltpu.VMEM((line, rows, width), bf),
            pltpu.VMEM((line, rows, width), bf),
            pltpu.VMEM((line, rows, width), bf),
            pltpu.VMEM((line, rows, lanes), f32),
            pltpu.VMEM((rows, max(hid, shared_hid)), bf),
            dma((7,)),
            dma((2,)),
            dma((2,)),
            dma((1,)),
            dma((1,)),
            dma((2,)),
            dma((2,)),
            dma((PIECES,)),
            dma((PIECES,)),
        ]
        + [dma((count,))] * 8
        + [dma((line,))] * 2
        + [dma((line, PIECES))] * 8,
        compiler_params=pltpu.CompilerParams(
            collective_id=0, has_side_effects=True, vmem_limit_bytes=60 * 1024 * 1024
        ),
    )(
        x_in, gate_b, gate_c, conv_taps, resid, jnp.stack([mix_gain, pre_gain, post_gain]),
        routes, route_weights, out_proj, expert_gate, expert_up, expert_down,
        shared_gate, shared_up, shared_down,
    )


def passed_along(shard, axis, by):
    size = lax.axis_size(axis)
    pairs = [(i, i + by) for i in range(size) if 0 <= i + by < size]
    return lax.ppermute(shard, axis, pairs)


def body(
    x_in,
    gate_b,
    gate_c,
    conv_taps,
    out_proj,
    mix_gain,
    resid,
    pre_gain,
    expert_gate,
    expert_up,
    expert_down,
    shared_gate,
    shared_up,
    shared_down,
    post_gain,
    routes,
    route_weights,
):
    group = lax.axis_size("sp")
    wide_slots = 3 * resid.shape[0] * routes.shape[1] // group
    if wide_slots > resid.shape[0] and group % 2 == 0 and lax.axis_size("tp") == 2 * 2:
        return fused_layer(
            x_in, gate_b, gate_c, conv_taps, out_proj, mix_gain, resid, pre_gain, expert_gate,
            expert_up, expert_down, shared_gate, shared_up, shared_down, post_gain, routes,
            route_weights,
        )
    row_count = x_in.shape[0]
    channels = x_in.shape[1]
    reach = conv_taps.shape[0] - 1
    edge_rows = jnp.concatenate([x_in[row_count - reach :], gate_c[row_count - reach :]], 1)
    arrived_edge = passed_along(edge_rows, "sp", 1)
    inputs = jnp.concatenate([arrived_edge[:, :channels], x_in], 0).astype(jnp.float32)
    gate_rows = jnp.concatenate([arrived_edge[:, channels:], gate_c], 0).astype(jnp.float32)
    mixed_in = inputs * gate_rows
    taps = conv_taps.astype(jnp.float32)
    convolved = jnp.zeros((row_count, channels), jnp.float32)
    for index in range(reach + 1):
        convolved = convolved + taps[index][None, :] * mixed_in[index : index + row_count]
    conv_out = (gate_b.astype(jnp.float32) * convolved).astype(jnp.bfloat16)
    width_all = out_proj.shape[1]
    full_rows = lax.all_to_all(conv_out, "tp", split_axis=0, concat_axis=1, tiled=True)
    projected = jnp.dot(
        full_rows,
        lax.all_gather(out_proj, "tp", axis=0, tiled=True),
        preferred_element_type=jnp.float32,
    )
    row_scale = lax.rsqrt(jnp.mean(projected * projected, axis=1, keepdims=True) + epsilon)
    resid1 = (
        resid.astype(jnp.float32) + projected * row_scale * mix_gain.astype(jnp.float32)
    ).astype(jnp.bfloat16)
    wide_resid = resid1.astype(jnp.float32)
    normed = (
        wide_resid
        * lax.rsqrt(jnp.mean(wide_resid * wide_resid, axis=1, keepdims=True) + epsilon)
        * pre_gain.astype(jnp.float32)
    ).astype(jnp.bfloat16)
    experts = lax.axis_size("sp")
    local_rows = resid.shape[0]
    top_count = routes.shape[1]
    capacity = 3 * local_rows * top_count // (2 * experts)
    flat_ids = routes.reshape(-1)
    onehot = (flat_ids[:, None] == jnp.arange(experts, dtype=jnp.int32)[None, :]).astype(jnp.int32)
    before = jnp.cumsum(onehot, axis=0) - onehot
    position = jnp.sum(before * onehot, axis=1)
    slot_index = flat_ids * capacity + position
    outgoing = (
        jnp.zeros((experts * capacity, width_all), jnp.bfloat16)
        .at[slot_index]
        .set(jnp.repeat(normed, top_count, axis=0))
    )
    received = lax.all_to_all(
        outgoing.reshape(experts, capacity, width_all),
        "sp",
        split_axis=0,
        concat_axis=0,
        tiled=True,
    )
    arrived = received.reshape(experts * capacity, width_all)
    gate_h = jnp.dot(arrived, expert_gate[0], preferred_element_type=jnp.float32)
    up_h = jnp.dot(arrived, expert_up[0], preferred_element_type=jnp.float32)
    hidden = (jax.nn.silu(gate_h) * up_h).astype(jnp.bfloat16)
    expert_out = jnp.dot(hidden, expert_down[0], preferred_element_type=jnp.float32).astype(
        jnp.bfloat16
    )
    returned = lax.all_to_all(
        expert_out.reshape(experts, capacity, width_all),
        "sp",
        split_axis=0,
        concat_axis=0,
        tiled=True,
    )
    returned = returned.reshape(experts * capacity, width_all)
    picked = returned[slot_index].astype(jnp.float32).reshape(local_rows, top_count, width_all)
    routed = jnp.einsum("tk,tkd->td", route_weights, picked)
    shared_g = jnp.dot(normed, shared_gate, preferred_element_type=jnp.float32)
    shared_u = jnp.dot(normed, shared_up, preferred_element_type=jnp.float32)
    shared_hidden = (jax.nn.silu(shared_g) * shared_u).astype(jnp.bfloat16)
    shared_out = jnp.dot(shared_hidden, shared_down, preferred_element_type=jnp.float32)
    branch = routed + shared_out
    factor = lax.rsqrt(jnp.mean(branch * branch, axis=1, keepdims=True) + epsilon)
    return (wide_resid + branch * factor * post_gain.astype(jnp.float32)[None, :]).astype(
        jnp.bfloat16
    )


def solution(mesh):
    return jax.shard_map(
        body,
        mesh=mesh,
        in_specs=(
            P("sp", "tp"),
            P("sp", "tp"),
            P("sp", "tp"),
            P(None, "tp"),
            P("tp", None),
            P(),
            P(("sp", "tp"), None),
            P(),
            P("sp", None, None),
            P("sp", None, None),
            P("sp", None, None),
            P(),
            P(),
            P(),
            P(),
            P(("sp", "tp"), None),
            P(("sp", "tp"), None),
        ),
        out_specs=P(("sp", "tp"), None),
        check_vma=False,
    )
```

```python
import functools

import jax
import jax.numpy as jnp
from jax import lax
from jax.experimental import pallas as pl
from jax.experimental.pallas import tpu as pltpu

P = jax.sharding.PartitionSpec
MESH = pl.DeviceIdType.MESH
epsilon = 1e-06
PIECES = 4
HALVES = 2
DIRECT = 2


def layer_kernel(
    line,
    x_ref,
    gate_b_ref,
    gate_c_ref,
    taps_ref,
    resid_ref,
    gains_ref,
    routes_ref,
    weights_ref,
    proj_ref,
    eg_ref,
    eu_ref,
    ed_ref,
    sg_ref,
    su_ref,
    sd_ref,
    out_ref,
    edge_x,
    edge_c,
    mixed,
    conv,
    conv_near,
    proj,
    part_out,
    part_in,
    projected,
    resid1,
    w_gate,
    w_up,
    w_down,
    s_gate,
    s_up,
    s_down,
    blocks,
    sums,
    shared,
    from_low,
    from_high,
    outgoing,
    shares,
    hidden,
    load_sem,
    e_send,
    e_recv,
    p_send,
    p_recv,
    c_send,
    c_recv,
    f_send,
    f_recv,
    wx_send,
    wx_recv,
    wn_send,
    wn_recv,
    wf_send,
    wf_recv,
    wr_send,
    wr_recv,
    t_send,
    t_recv,
    gu_send,
    gu_recv,
    gd_send,
    gd_recv,
    ru_send,
    ru_recv,
    rd_send,
    rd_recv,
):
    sp = lax.axis_index("sp")
    tp = lax.axis_index("tp")
    sp_size = lax.axis_size("sp")
    tp_size = lax.axis_size("tp")
    z = sp // 2
    x = sp % 2
    last = line - 1
    mate = z * 2 + 1 - x
    near = (tp // 2) * 2 + 1 - tp % 2
    far = (tp + 2) % tp_size
    near_far = (near + 2) % tp_size
    rows, width = resid_ref.shape
    step_rows = rows // PIECES
    hid = w_gate.shape[2]
    shared_hid = s_gate.shape[1]

    barrier = pltpu.get_barrier_semaphore()
    for k in range(1, sp_size):
        pl.semaphore_signal(barrier, inc=1, device_id=((sp + k) % sp_size, tp), device_id_type=MESH)
    for k in range(1, tp_size):
        pl.semaphore_signal(barrier, inc=1, device_id=(sp, (tp + k) % tp_size), device_id_type=MESH)

    loads = [
        pltpu.make_async_copy(src, dst, load_sem.at[n])
        for n, (src, dst) in enumerate(
            (
                (eg_ref.at[0], w_gate.at[0]),
                (eu_ref.at[0], w_up.at[0]),
                (ed_ref.at[0], w_down.at[0]),
                (sg_ref, s_gate),
                (su_ref, s_up),
                (sd_ref, s_down),
                (proj_ref, proj.at[0]),
            )
        )
    ]
    loads[-1].start()
    for load in loads[:-1]:
        load.start()

    all_rows, channels = x_ref.shape
    reach = taps_ref.shape[0] - 1
    pad = edge_x.shape[0]
    mixed[pad:] = x_ref[...].astype(jnp.float32) * gate_c_ref[...].astype(jnp.float32)

    def edge_copy(n):
        source, landing = ((x_ref, edge_x), (gate_c_ref, edge_c))[n]
        return pltpu.make_async_remote_copy(
            src_ref=source.at[pl.ds(all_rows - pad, pad)],
            dst_ref=landing,
            send_sem=e_send.at[n],
            recv_sem=e_recv.at[n],
            device_id=((sp + 1) % sp_size, tp),
            device_id_type=MESH,
        )

    proj_copy = pltpu.make_async_remote_copy(
        src_ref=proj_ref,
        dst_ref=proj.at[1],
        send_sem=p_send.at[0],
        recv_sem=p_recv.at[0],
        device_id=(sp, near),
        device_id_type=MESH,
    )

    def block_rows(owner):
        return pl.ds(pl.multiple_of(owner * rows, rows), rows)

    def conv_copy(n):
        return pltpu.make_async_remote_copy(
            src_ref=conv.at[block_rows((near, near_far)[n])],
            dst_ref=conv_near.at[n],
            send_sem=c_send.at[n],
            recv_sem=c_recv.at[n],
            device_id=(sp, near),
            device_id_type=MESH,
        )

    part_cols = width // PIECES

    def part_copy(j):
        cols = pl.ds(pl.multiple_of(j * part_cols, part_cols), part_cols)
        return pltpu.make_async_remote_copy(
            src_ref=part_out.at[:, cols],
            dst_ref=part_in.at[:, cols],
            send_sem=f_send.at[j],
            recv_sem=f_recv.at[j],
            device_id=(sp, far),
            device_id_type=MESH,
        )

    pl.semaphore_wait(barrier, sp_size - 1 + tp_size - 1)

    @pl.when(sp < sp_size - 1)
    def _():
        edge_copy(0).start()
        edge_copy(1).start()

    proj_copy.start()

    pieces = []
    for ref, held in ((eg_ref, w_gate), (eu_ref, w_up), (ed_ref, w_down)):
        size = ref.shape[1] // tp_size // HALVES
        for h in range(HALVES):
            pieces.append((ref, held, size, h))

    def span(owner, n):
        _, _, size, h = pieces[n]
        return pl.ds(pl.multiple_of((owner * HALVES + h) * size, size), size)

    def hop(n, owner, target, send, recv, first=False):
        ref, held, _, _ = pieces[n]
        where = span(owner, n)
        return pltpu.make_async_remote_copy(
            src_ref=ref.at[0, where] if first else held.at[1, where],
            dst_ref=held.at[1, where],
            send_sem=send.at[n],
            recv_sem=recv.at[n],
            device_id=target,
            device_id_type=MESH,
        )

    def x_hop(n):
        return hop(n, tp, (mate, tp), wx_send, wx_recv, True)

    def near_hop(n, owner):
        return hop(n, owner, (sp, near), wn_send, wn_recv)

    def far_hop(n, owner):
        return hop(n, owner, (sp, far), wf_send, wf_recv)

    def direct_hop(n):
        return hop(n, far, (mate, tp), wf_send, wf_recv, True)

    def relay_hop(n, owner):
        return hop(n, owner, (sp, near), wr_send, wr_recv)

    count = len(pieces)

    def line_copy(source, landing, b, c, up, send, recv):
        part = pl.ds(pl.multiple_of(c * step_rows, step_rows), step_rows)
        return pltpu.make_async_remote_copy(
            src_ref=source.at[b, part],
            dst_ref=landing.at[b, part],
            send_sem=send.at[b, c],
            recv_sem=recv.at[b, c],
            device_id=((z + (1 if up else -1)) * 2 + x, tp),
            device_id_type=MESH,
        )

    def go_up(b, c):
        return line_copy(blocks, blocks, b, c, True, gu_send, gu_recv)

    def go_down(b, c):
        return line_copy(blocks, blocks, b, c, False, gd_send, gd_recv)

    def back_up(b, c):
        return line_copy(outgoing, from_low, b, c, True, ru_send, ru_recv)

    def back_down(b, c):
        return line_copy(outgoing, from_high, b, c, False, rd_send, rd_recv)

    def share_copy(k, source):
        return pltpu.make_async_remote_copy(
            src_ref=shares.at[source],
            dst_ref=shares.at[source],
            send_sem=t_send.at[k],
            recv_sem=t_recv.at[source],
            device_id=(((z + k) % line) * 2 + x, tp),
            device_id_type=MESH,
        )

    for n in range(count):
        x_hop(n).start()
    for n in range(count - DIRECT, count):
        direct_hop(n).start()

    lanes = lax.broadcasted_iota(jnp.int32, (rows, shares.shape[2]), 1)
    table = jnp.zeros((rows, shares.shape[2]), jnp.float32)
    for k in range(routes_ref.shape[1]):
        table += jnp.where(lanes == routes_ref[:, k : k + 1], weights_ref[:, k : k + 1], 0.0)
    shares[z] = table

    @pl.when(sp > 0)
    def _():
        edge_copy(0).wait_recv()
        edge_copy(1).wait_recv()
        mixed[:pad] = edge_x[...].astype(jnp.float32) * edge_c[...].astype(jnp.float32)

    @pl.when(sp == 0)
    def _():
        mixed[:pad] = jnp.zeros((pad, channels), jnp.float32)

    convolved = jnp.zeros((all_rows, channels), jnp.float32)
    for k in range(reach + 1):
        begin = pad - reach + k
        convolved += taps_ref[k : k + 1].astype(jnp.float32) * mixed[begin : begin + all_rows]
    conv[...] = (gate_b_ref[...].astype(jnp.float32) * convolved).astype(jnp.bfloat16)
    conv_copy(1).start()
    conv_copy(0).start()
    for k in range(1, line):
        share_copy(k, z).start()
    loads[-1].wait()
    proj_copy.wait_recv()

    def project(n, owner, cols):
        return jnp.dot(
            conv[block_rows(owner)], proj[0, :, cols], preferred_element_type=jnp.float32
        ) + jnp.dot(conv_near[n], proj[1, :, cols], preferred_element_type=jnp.float32)

    conv_copy(1).wait_recv()

    @pl.loop(0, PIECES)
    def _(j):
        cols = pl.ds(pl.multiple_of(j * part_cols, part_cols), part_cols)
        part_out[:, cols] = project(1, far, cols).astype(jnp.bfloat16)
        part_copy(j).start()

    conv_copy(0).wait_recv()

    @pl.loop(0, PIECES)
    def _(j):
        cols = pl.ds(pl.multiple_of(j * part_cols, part_cols), part_cols)
        projected[:, cols] = project(0, tp, cols)

    sums[...] = jnp.zeros_like(sums)

    def spread(n):
        x_hop(n).wait_recv()
        if n < count - DIRECT:
            far_hop(n, tp).start()
        near_hop(n, tp).start()

    for n in range(count // 2):
        spread(n)

    @pl.loop(0, PIECES)
    def _(j):
        cols = pl.ds(pl.multiple_of(j * part_cols, part_cols), part_cols)
        part_copy(j).wait_recv()
        projected[:, cols] += part_in[:, cols].astype(jnp.float32)

    def send_block(c):
        @pl.when(z < last)
        def _():
            go_up(z, c).start()

        @pl.when(z > 0)
        def _():
            go_down(z, c).start()

    for c in range(PIECES):
        part = pl.ds(c * step_rows, step_rows)
        block = projected[part]
        scale = lax.rsqrt(jnp.mean(block * block, axis=1, keepdims=True) + epsilon)
        mid = (
            resid_ref[part].astype(jnp.float32)
            + block * scale * gains_ref[0:1].astype(jnp.float32)
        ).astype(jnp.bfloat16)
        resid1[part] = mid
        wide = mid.astype(jnp.float32)
        normal = lax.rsqrt(jnp.mean(wide * wide, axis=1, keepdims=True) + epsilon)
        blocks[z, part] = (wide * normal * gains_ref[1:2].astype(jnp.float32)).astype(jnp.bfloat16)
        if c > 0:
            send_block(c - 1)
    send_block(PIECES - 1)

    def apply(b, i):
        expert = z * 2 + x + i * (1 - 2 * x)

        @pl.loop(0, hid // 256)
        def _(j):
            cols = pl.ds(pl.multiple_of(j * 256, 256), 256)
            gate = jnp.dot(blocks[b], w_gate[i, :, cols], preferred_element_type=jnp.float32)
            up = jnp.dot(blocks[b], w_up[i, :, cols], preferred_element_type=jnp.float32)
            hidden[:, cols] = (jax.nn.silu(gate) * up).astype(jnp.bfloat16)

        share = jnp.sum(jnp.where(lanes == expert, shares[b], 0.0), axis=1, keepdims=True)

        @pl.loop(0, width // 512)
        def _(j):
            cols = pl.ds(pl.multiple_of(j * 512, 512), 512)
            made = jnp.dot(hidden[...], w_down[i, :, cols], preferred_element_type=jnp.float32)
            made = made.astype(jnp.bfloat16).astype(jnp.float32)
            sums[b, :, cols] += jnp.where(share > 0.0, share * made, 0.0)

    def receive(t):
        @pl.loop(0, PIECES)
        def _(c):
            @pl.when(z - t >= 0)
            def _():
                go_up(z - t, c).wait_recv()

                @pl.when(z < last)
                def _():
                    go_up(z - t, c).start()

            @pl.when(z + t <= last)
            def _():
                go_down(z + t, c).wait_recv()

                @pl.when(z > 0)
                def _():
                    go_down(z + t, c).start()

    def apply_pair(t, i):
        @pl.loop(0, 2)
        def _(side):
            b = z - t + side * 2 * t

            @pl.when((b >= 0) & (b <= last))
            def _():
                apply(b, i)

    def give_back(t):
        p_up = t - z
        p_down = t - (last - z)
        b_up = (p_up + last) % last + 1
        b_down = last - ((p_down + last) % last + 1)
        send_up = (p_up >= 1) & (p_up <= last) & (b_up > z)
        send_down = (p_down >= 1) & (p_down <= last) & (b_down < z)

        @pl.loop(0, PIECES)
        def _(c):
            part = pl.ds(pl.multiple_of(c * step_rows, step_rows), step_rows)

            @pl.when(send_up)
            def _():
                @pl.when(z > 0)
                def _():
                    back_up(b_up, c).wait_recv()
                    sums[b_up, part] += from_low[b_up, part].astype(jnp.float32)

                outgoing[b_up, part] = sums[b_up, part].astype(jnp.bfloat16)
                back_up(b_up, c).start()

            @pl.when(send_down)
            def _():
                @pl.when(z < last)
                def _():
                    back_down(b_down, c).wait_recv()
                    sums[b_down, part] += from_high[b_down, part].astype(jnp.float32)

                outgoing[b_down, part] = sums[b_down, part].astype(jnp.bfloat16)
                back_down(b_down, c).start()

    for load in loads[:3]:
        load.wait()
    apply(z, 0)
    for load in loads[3:-1]:
        load.wait()
    s_g = jnp.dot(blocks[z], s_gate[...], preferred_element_type=jnp.float32)
    s_u = jnp.dot(blocks[z], s_up[...], preferred_element_type=jnp.float32)
    s_h = (jax.nn.silu(s_g) * s_u).astype(jnp.bfloat16)
    hidden[:, :shared_hid] = s_h

    @pl.loop(0, width // 512)
    def _(j):
        cols = pl.ds(pl.multiple_of(j * 512, 512), 512)
        shared[:, cols] = jnp.dot(
            hidden[:, :shared_hid], s_down[:, cols], preferred_element_type=jnp.float32
        )

    for n in range(count // 2, count):
        spread(n)
    receive(1)
    for k in range(1, line):
        share_copy(k, (z + k) % line).wait_recv()
    apply_pair(1, 0)

    def relay(n):
        far_hop(n, far).wait_recv()
        relay_hop(n, far).start()

    for n in range(2 * count // 3):
        relay(n)
    for t in range(2, last):
        receive(t)
        apply_pair(t, 0)
    for n in range(2 * count // 3, count):
        relay(n)
    for n in range(count):
        near_hop(n, near).wait_recv()
        relay_hop(n, near_far).wait_recv()

    @pl.loop(2, last)
    def _(t):
        apply_pair(t, 1)

    give_back(1)
    apply_pair(1, 1)
    receive(last)
    apply_pair(last, 0)
    apply_pair(last, 1)
    give_back(2)
    apply(z, 1)

    @pl.loop(3, 2 * last - 1)
    def _(t):
        give_back(t)

    @pl.loop(0, PIECES)
    def _(c):
        part = pl.ds(pl.multiple_of(c * step_rows, step_rows), step_rows)

        @pl.when(z > 0)
        def _():
            back_up(z, c).wait_recv()
            sums[z, part] += from_low[z, part].astype(jnp.float32)

        @pl.when(z < last)
        def _():
            back_down(z, c).wait_recv()
            sums[z, part] += from_high[z, part].astype(jnp.float32)

        branch = sums[z, part] + shared[part]
        factor = lax.rsqrt(jnp.mean(branch * branch, axis=1, keepdims=True) + epsilon)
        out_ref[part] = (
            resid1[part].astype(jnp.float32)
            + branch * factor * gains_ref[2:3].astype(jnp.float32)
        ).astype(jnp.bfloat16)

    @pl.when(sp < sp_size - 1)
    def _():
        edge_copy(0).wait_send()
        edge_copy(1).wait_send()

    proj_copy.wait_send()
    conv_copy(0).wait_send()
    conv_copy(1).wait_send()
    for j in range(PIECES):
        part_copy(j).wait_send()
    for n in range(count):
        x_hop(n).wait_send()
        near_hop(n, tp).wait_send()
        far_hop(n, tp).wait_send()
        relay_hop(n, far).wait_send()
    for k in range(1, line):
        share_copy(k, z).wait_send()

    @pl.loop(0, PIECES)
    def _(c):
        @pl.loop(0, line)
        def _(b):
            @pl.when((b <= z) & (z < last))
            def _():
                go_up(b, c).wait_send()

            @pl.when((b >= z) & (z > 0))
            def _():
                go_down(b, c).wait_send()

            @pl.when(b > z)
            def _():
                back_up(b, c).wait_send()

            @pl.when(b < z)
            def _():
                back_down(b, c).wait_send()


def fused_layer(
    x_in, gate_b, gate_c, conv_taps, out_proj, mix_gain, resid, pre_gain, expert_gate, expert_up,
    expert_down, shared_gate, shared_up, shared_down, post_gain, routes, route_weights,
):
    experts = lax.axis_size("sp")
    line = experts // 2
    all_rows, channels = x_in.shape
    rows, width = resid.shape
    hid = expert_gate.shape[2]
    shared_hid = shared_gate.shape[1]
    dma = pltpu.SemaphoreType.DMA
    count = 3 * HALVES
    bf, f32 = jnp.bfloat16, jnp.float32
    vmem = pl.BlockSpec(memory_space=pltpu.VMEM)
    hbm = pl.BlockSpec(memory_space=pltpu.HBM)
    lanes = 128 * (-(-experts // 128))
    pad = 16 * (-(-(conv_taps.shape[0] - 1) // 16))
    return pl.pallas_call(
        functools.partial(layer_kernel, line),
        out_shape=jax.ShapeDtypeStruct((rows, width), bf),
        in_specs=[vmem] * 8 + [hbm] * 7,
        out_specs=vmem,
        scratch_shapes=[
            pltpu.VMEM((pad, channels), bf),
            pltpu.VMEM((pad, channels), bf),
            pltpu.VMEM((pad + all_rows, channels), f32),
            pltpu.VMEM((all_rows, channels), bf),
            pltpu.VMEM((2, rows, channels), bf),
            pltpu.VMEM((2, channels, width), bf),
            pltpu.VMEM((rows, width), bf),
            pltpu.VMEM((rows, width), bf),
            pltpu.VMEM((rows, width), f32),
            pltpu.VMEM((rows, width), bf),
            pltpu.VMEM((2, width, hid), bf),
            pltpu.VMEM((2, width, hid), bf),
            pltpu.VMEM((2, hid, width), bf),
            pltpu.VMEM((width, shared_hid), bf),
            pltpu.VMEM((width, shared_hid), bf),
            pltpu.VMEM((shared_hid, width), bf),
            pltpu.VMEM((line, rows, width), bf),
            pltpu.VMEM((line, rows, width), f32),
            pltpu.VMEM((rows, width), f32),
            pltpu.VMEM((line, rows, width), bf),
            pltpu.VMEM((line, rows, width), bf),
            pltpu.VMEM((line, rows, width), bf),
            pltpu.VMEM((line, rows, lanes), f32),
            pltpu.VMEM((rows, max(hid, shared_hid)), bf),
            dma((7,)),
            dma((2,)),
            dma((2,)),
            dma((1,)),
            dma((1,)),
            dma((2,)),
            dma((2,)),
            dma((PIECES,)),
            dma((PIECES,)),
        ]
        + [dma((count,))] * 8
        + [dma((line,))] * 2
        + [dma((line, PIECES))] * 8,
        compiler_params=pltpu.CompilerParams(
            collective_id=0, has_side_effects=True, vmem_limit_bytes=60 * 1024 * 1024
        ),
    )(
        x_in, gate_b, gate_c, conv_taps, resid, jnp.stack([mix_gain, pre_gain, post_gain]),
        routes, route_weights, out_proj, expert_gate, expert_up, expert_down,
        shared_gate, shared_up, shared_down,
    )


def passed_along(shard, axis, by):
    size = lax.axis_size(axis)
    pairs = [(i, i + by) for i in range(size) if 0 <= i + by < size]
    return lax.ppermute(shard, axis, pairs)


def body(
    x_in,
    gate_b,
    gate_c,
    conv_taps,
    out_proj,
    mix_gain,
    resid,
    pre_gain,
    expert_gate,
    expert_up,
    expert_down,
    shared_gate,
    shared_up,
    shared_down,
    post_gain,
    routes,
    route_weights,
):
    group = lax.axis_size("sp")
    wide_slots = 3 * resid.shape[0] * routes.shape[1] // group
    if wide_slots > resid.shape[0] and group % 2 == 0 and lax.axis_size("tp") == 2 * 2:
        return fused_layer(
            x_in, gate_b, gate_c, conv_taps, out_proj, mix_gain, resid, pre_gain, expert_gate,
            expert_up, expert_down, shared_gate, shared_up, shared_down, post_gain, routes,
            route_weights,
        )
    row_count = x_in.shape[0]
    channels = x_in.shape[1]
    reach = conv_taps.shape[0] - 1
    edge_rows = jnp.concatenate([x_in[row_count - reach :], gate_c[row_count - reach :]], 1)
    arrived_edge = passed_along(edge_rows, "sp", 1)
    inputs = jnp.concatenate([arrived_edge[:, :channels], x_in], 0).astype(jnp.float32)
    gate_rows = jnp.concatenate([arrived_edge[:, channels:], gate_c], 0).astype(jnp.float32)
    mixed_in = inputs * gate_rows
    taps = conv_taps.astype(jnp.float32)
    convolved = jnp.zeros((row_count, channels), jnp.float32)
    for index in range(reach + 1):
        convolved = convolved + taps[index][None, :] * mixed_in[index : index + row_count]
    conv_out = (gate_b.astype(jnp.float32) * convolved).astype(jnp.bfloat16)
    width_all = out_proj.shape[1]
    full_rows = lax.all_to_all(conv_out, "tp", split_axis=0, concat_axis=1, tiled=True)
    projected = jnp.dot(
        full_rows,
        lax.all_gather(out_proj, "tp", axis=0, tiled=True),
        preferred_element_type=jnp.float32,
    )
    row_scale = lax.rsqrt(jnp.mean(projected * projected, axis=1, keepdims=True) + epsilon)
    resid1 = (
        resid.astype(jnp.float32) + projected * row_scale * mix_gain.astype(jnp.float32)
    ).astype(jnp.bfloat16)
    wide_resid = resid1.astype(jnp.float32)
    normed = (
        wide_resid
        * lax.rsqrt(jnp.mean(wide_resid * wide_resid, axis=1, keepdims=True) + epsilon)
        * pre_gain.astype(jnp.float32)
    ).astype(jnp.bfloat16)
    experts = lax.axis_size("sp")
    local_rows = resid.shape[0]
    top_count = routes.shape[1]
    capacity = 3 * local_rows * top_count // (2 * experts)
    flat_ids = routes.reshape(-1)
    onehot = (flat_ids[:, None] == jnp.arange(experts, dtype=jnp.int32)[None, :]).astype(jnp.int32)
    before = jnp.cumsum(onehot, axis=0) - onehot
    position = jnp.sum(before * onehot, axis=1)
    slot_index = flat_ids * capacity + position
    outgoing = (
        jnp.zeros((experts * capacity, width_all), jnp.bfloat16)
        .at[slot_index]
        .set(jnp.repeat(normed, top_count, axis=0))
    )
    received = lax.all_to_all(
        outgoing.reshape(experts, capacity, width_all),
        "sp",
        split_axis=0,
        concat_axis=0,
        tiled=True,
    )
    arrived = received.reshape(experts * capacity, width_all)
    gate_h = jnp.dot(arrived, expert_gate[0], preferred_element_type=jnp.float32)
    up_h = jnp.dot(arrived, expert_up[0], preferred_element_type=jnp.float32)
    hidden = (jax.nn.silu(gate_h) * up_h).astype(jnp.bfloat16)
    expert_out = jnp.dot(hidden, expert_down[0], preferred_element_type=jnp.float32).astype(
        jnp.bfloat16
    )
    returned = lax.all_to_all(
        expert_out.reshape(experts, capacity, width_all),
        "sp",
        split_axis=0,
        concat_axis=0,
        tiled=True,
    )
    returned = returned.reshape(experts * capacity, width_all)
    picked = returned[slot_index].astype(jnp.float32).reshape(local_rows, top_count, width_all)
    routed = jnp.einsum("tk,tkd->td", route_weights, picked)
    shared_g = jnp.dot(normed, shared_gate, preferred_element_type=jnp.float32)
    shared_u = jnp.dot(normed, shared_up, preferred_element_type=jnp.float32)
    shared_hidden = (jax.nn.silu(shared_g) * shared_u).astype(jnp.bfloat16)
    shared_out = jnp.dot(shared_hidden, shared_down, preferred_element_type=jnp.float32)
    branch = routed + shared_out
    factor = lax.rsqrt(jnp.mean(branch * branch, axis=1, keepdims=True) + epsilon)
    return (wide_resid + branch * factor * post_gain.astype(jnp.float32)[None, :]).astype(
        jnp.bfloat16
    )


def solution(mesh):
    return jax.shard_map(
        body,
        mesh=mesh,
        in_specs=(
            P("sp", "tp"),
            P("sp", "tp"),
            P("sp", "tp"),
            P(None, "tp"),
            P("tp", None),
            P(),
            P(("sp", "tp"), None),
            P(),
            P("sp", None, None),
            P("sp", None, None),
            P("sp", None, None),
            P(),
            P(),
            P(),
            P(),
            P(("sp", "tp"), None),
            P(("sp", "tp"), None),
        ),
        out_specs=P(("sp", "tp"), None),
        check_vma=False,
    )
```
